32 devices in a mesh: fs: 4 (over z), rep: 4 (over y, x), tp: 2 (over core).
Axes of the slice: x: 2, y: 2, z: 4, core: 2. Of those that a mesh axis runs over, the one named last changes fastest.
Arguments:
- normed: bfloat16 [10240, 2048], P(('fs', 'rep')), may hold values from -150 to 150
- rec_cot: bfloat16 [10240, 2048], P(('fs', 'rep'), 'tp'), may hold values from -1.4823177 to 1.4823177
- conv_out: bfloat16 [10240, 2048], P(('fs', 'rep'), 'tp'), may hold values from -6 to 6
- gate_cot: bfloat16 [10240, 2048], P(('fs', 'rep'), 'tp'), may hold values from -0.05908203 to 0.05908203
- rec_weight: float32 [2048, 2048], P('fs', 'tp'), may hold values from -0.125 to 0.125
- rec_moment: float32 [2048, 2048], P('fs', 'tp'), may hold values from -6 to 6
- rec_right: bfloat16 [2048, 256], P('tp'), may hold values from -1 to 2
- gate_weight: float32 [8, 256, 256], P('tp', 'fs'), may hold values from -0.375 to 0.375
- gate_moment: float32 [8, 256, 256], P('tp', 'fs'), may hold values from -6 to 6
- gate_left: bfloat16 [8, 256, 256], P('tp', 'fs'), may hold values from -1 to 2
- gate_right: bfloat16 [8, 256, 256], P('tp'), may hold values from -1 to 2
Outputs:
- rec_weight_new: float32 [2048, 2048], P('fs', 'tp')
- rec_moment_new: float32 [2048, 2048], P('fs', 'tp')
- rec_step: float32 [2048, 2048], P('fs', 'tp')
- rec_copy: bfloat16 [2048, 2048], P('fs', 'tp')
- gate_weight_new: float32 [8, 256, 256], P('tp', 'fs')
- gate_moment_new: float32 [8, 256, 256], P('tp', 'fs')
- gate_step: float32 [8, 256, 256], P('tp', 'fs')
- gate_copy: bfloat16 [8, 256, 256], P('tp', 'fs')
The draws below stay inside these ranges and needn't reach their ends.
All inputs are finite; a program needn't handle non-finite values.
Results may differ from the reference program's by a relative error of at most 0.001.
Values sent between devices are 32-bit elements; how exact they have to be, the bound alone decides.
A program may use at most 64 MiB of HBM per device.

```python
import jax
import jax.numpy as jnp
from jax import lax

D = 2048
D_RNN = 2048
HEADS = 8
BLK = 256
TOKENS = 10240


def rising_scales(key, column_count):
    position = jnp.arange(column_count, dtype=jnp.float32) / column_count
    jitter = jnp.exp(jax.random.uniform(key, (column_count,), jnp.float32, 0.0, jnp.log(3.0)))
    return jnp.exp(jnp.log(4.0) * position) * jitter


def token_matrix(key, column_count, overall):
    key_list = jax.random.split(key, 2)
    scales = rising_scales(key_list[0], column_count) * overall
    values = jnp.clip(jax.random.normal(key_list[1], (TOKENS, column_count), jnp.float32), -6.0, 6.0)
    return values * scales


def identity_plus(key, count, block_size):
    noise = jnp.clip(jax.random.normal(key, (count, block_size, block_size), jnp.float32), -4.0, 4.0)
    symmetric = (noise + jnp.swapaxes(noise, 1, 2)) * (0.5 / jnp.sqrt(2.0 * block_size))
    result = jnp.eye(block_size, dtype=jnp.float32)[None] + symmetric
    return jnp.clip(result, -1.0, 2.0)


def draw_normed(key, part):
    return token_matrix(jax.random.fold_in(key, 11), D, 1.0).astype(jnp.bfloat16)


def draw_rec_cot(key, part):
    return token_matrix(jax.random.fold_in(key, 12), D_RNN, TOKENS ** (-0.5)).astype(jnp.bfloat16)


def draw_rec_right(key, part):
    blocks = identity_plus(jax.random.fold_in(key, 13), D_RNN // BLK, BLK)
    return blocks.reshape(D_RNN, BLK).astype(jnp.bfloat16)


def draw_gate_left(key, part):
    return identity_plus(jax.random.fold_in(key, 14), HEADS, BLK).astype(jnp.bfloat16)


def draw_gate_right(key, part):
    return identity_plus(jax.random.fold_in(key, 15), HEADS, BLK).astype(jnp.bfloat16)


def steps_of(stream_key, dims, pieces, low, high):
    loudness, own = 1.0, jax.random.fold_in(stream_key, 6)
    for dim, parts in pieces:
        draws = jnp.exp(jax.random.uniform(jax.random.fold_in(own, dim), (parts,), jnp.float32, low / len(pieces), high / len(pieces)))
        loudness = loudness * jnp.repeat(draws, dims[dim] // parts).reshape([-1 if axis == dim else 1 for axis in range(len(dims))])
    return loudness


def scatter_about(own_key, extent, scale, bound, pieces=(), kind=jnp.bfloat16):
    values = scale * jax.random.normal(own_key, extent, jnp.float32)
    if pieces:
        values = values * steps_of(own_key, extent, pieces, -0.22, 0.18)
    return jnp.clip(values, -bound, bound).astype(kind)


def setup_inputs(seed: int = 0) -> dict:
    splits = jax.random.split(jax.random.key(seed), 12)
    return {
        "normed": draw_normed(jax.random.fold_in(splits[11], 71), 0),
        "rec_cot": draw_rec_cot(jax.random.fold_in(splits[11], 71), 0),
        "conv_out": scatter_about(splits[2], (TOKENS, D_RNN), 1.0, 6.0, ((0, 16), (1, 2))),
        "gate_cot": scatter_about(splits[3], (TOKENS, D_RNN), (TOKENS ** -0.5), 0.05908203, ((0, 16), (1, 2))),
        "rec_weight": scatter_about(splits[4], (D, D_RNN), D ** -0.5, 0.125, ((0, 4), (1, 2)), jnp.float32),
        "rec_moment": scatter_about(splits[5], (D, D_RNN), 1.0, 6.0, ((0, 4), (1, 2)), jnp.float32),
        "rec_right": draw_rec_right(jax.random.fold_in(splits[11], 71), 0),
        "gate_weight": scatter_about(splits[7], (HEADS, BLK, BLK), BLK ** -0.5, 0.375, ((0, 2), (1, 4)), jnp.float32),
        "gate_moment": scatter_about(splits[8], (HEADS, BLK, BLK), 1.0, 6.0, ((0, 2), (1, 4)), jnp.float32),
        "gate_left": draw_gate_left(jax.random.fold_in(splits[11], 71), 0),
        "gate_right": draw_gate_right(jax.random.fold_in(splits[11], 71), 0),
    }


BETA = 0.9
LEARN_RATE = 0.02
EPSILON = 1e-06

def precondition_right(gradient, factor):
    row_count = gradient.shape[0]
    block_size = factor.shape[1]
    blocks = factor.shape[0] // block_size
    shaped = gradient.reshape(row_count, blocks, block_size)
    factors = factor.astype(jnp.float32).reshape(blocks, block_size, block_size)
    result = jnp.einsum('rbi,bij->rbj', shaped, factors, precision=lax.Precision.HIGHEST)
    return result.reshape(row_count, blocks * block_size)

def apply_update(weight, moment, precond, gradient):
    new_moment = BETA * moment + precond
    scale = jnp.sqrt(jnp.sum(gradient * gradient)) / jnp.sqrt(jnp.sum(new_moment * new_moment) + EPSILON)
    step_taken = LEARN_RATE * scale * new_moment
    new_weight = weight - step_taken
    return (new_weight, new_moment, step_taken, new_weight.astype(jnp.bfloat16))

def reference(normed, rec_cot, conv_out, gate_cot, rec_weight, rec_moment, rec_right, gate_weight, gate_moment, gate_left, gate_right):
    rec_grad = lax.dot_general(normed, rec_cot, (((0,), (0,)), ((), ())), preferred_element_type=jnp.float32)
    rec_pre = precondition_right(rec_grad, rec_right)
    conv_blocks = conv_out.astype(jnp.float32).reshape(TOKENS, HEADS, BLK)
    cot_blocks = gate_cot.astype(jnp.float32).reshape(TOKENS, HEADS, BLK)
    gate_grad = jnp.einsum('thi,thj->hij', conv_blocks, cot_blocks)
    right_done = jnp.einsum('hij,hjk->hik', gate_grad, gate_right.astype(jnp.float32), precision=lax.Precision.HIGHEST)
    gate_pre = jnp.einsum('hij,hjk->hik', gate_left.astype(jnp.float32), right_done, precision=lax.Precision.HIGHEST)
    rec_new, rec_mom, rec_taken, rec_low = apply_update(rec_weight, rec_moment, rec_pre, rec_grad)
    gate_new, gate_mom, gate_taken, gate_low = apply_update(gate_weight, gate_moment, gate_pre, gate_grad)
    return (rec_new, rec_mom, rec_taken, rec_low, gate_new, gate_mom, gate_taken, gate_low)
```

```python
import functools

import jax
import jax.numpy as jnp
from jax import lax
from jax.experimental import pallas as pl
from jax.experimental.pallas import tpu as pltpu
from jax.sharding import PartitionSpec as P

BETA = 0.9
LEARN_RATE = 0.02
EPSILON = 1e-06
MESH = pl.DeviceIdType.MESH
LANES = 128


def split_dot(value, factor):
    high = value.astype(jnp.bfloat16)
    low = (value - high.astype(jnp.float32)).astype(jnp.bfloat16)
    return jnp.dot(high, factor, preferred_element_type=jnp.float32) + jnp.dot(
        low, factor, preferred_element_type=jnp.float32
    )


def split_dot_left(factor, value):
    high = value.astype(jnp.bfloat16)
    low = (value - high.astype(jnp.float32)).astype(jnp.bfloat16)
    return jnp.dot(factor, high, preferred_element_type=jnp.float32) + jnp.dot(
        factor, low, preferred_element_type=jnp.float32
    )


def token_dot(left, right):
    return lax.dot_general(left, right, (((0,), (0,)), ((), ())), preferred_element_type=jnp.float32)


def folded_squares(value):
    squares = value * value
    rows, width = squares.shape
    total = jnp.sum(squares.reshape(rows // 8, 8, width), axis=0)
    result = total[:, :LANES]
    for start in range(LANES, width, LANES):
        result = result + total[:, start : start + LANES]
    return result


def kernel(
    fs_size, tp_size, halves,
    normed, rec_cot, conv_out, gate_cot, rec_moment, rec_right, gate_moment, gate_left, gate_right,
    rec_pre, gate_pre, scales,
    part, first, second, along, grad,
    gate_part, gate_first, gate_second, gate_along, gate_grad,
    sums, sums_fs, sums_tp,
    pair_send, pair_recv, fs_send, fs_recv, sum_send, sum_recv,
):
    fs, rep, tp = lax.axis_index("fs"), lax.axis_index("rep"), lax.axis_index("tp")
    bits = (lax.rem(rep, 2), rep // 2)
    partners = (rep + 1 - 2 * bits[0], rep + 2 - 4 * bits[1])
    fs_peers = [lax.rem(fs + step, fs_size) for step in range(1, fs_size)]
    tp_peers = [lax.rem(tp + step, tp_size) for step in range(1, tp_size)]

    barrier = pltpu.get_barrier_semaphore()
    peers = [{"rep": p} for p in partners] + [{"fs": p} for p in fs_peers] + [{"tp": p} for p in tp_peers]
    for peer in peers:
        pl.semaphore_signal(barrier, inc=1, device_id=peer, device_id_type=MESH)

    chunks = part.shape[0]
    width = part.shape[-1]
    quarter = part.shape[-2]
    half_rows = 8 * quarter
    fs_rows = halves * half_rows
    blocks = gate_part.shape[3]
    gate_rows = gate_part.shape[4]
    unit_count = chunks + 1
    sums[...] = jnp.zeros_like(sums)

    def remote(source, target, send, recv, peer):
        return pltpu.make_async_remote_copy(
            src_ref=source, dst_ref=target, send_sem=send, recv_sem=recv,
            device_id=peer, device_id_type=MESH,
        )

    def views(unit):
        if unit == 0:
            return gate_part, gate_first, gate_second, gate_along, gate_grad
        k = unit - 1
        return part.at[k], first.at[k], second.at[k], along.at[k], grad.at[k]

    def mine(stream):
        return bits[stream], bits[1 - stream]

    def pair_copy(unit, stream, stage):
        p, one, two, _, g = views(unit)
        a, b = mine(stream)
        side = stream if stage in (0, 3) else 1 - stream
        if stage == 0:
            source, target = p.at[stream, 1 - a], one.at[stream]
        elif stage == 1:
            source, target = p.at[stream, a, 1 - b], two.at[stream]
        elif stage == 2:
            source = target = g.at[stream, a, b]
        else:
            source = target = g.at[stream, a]
        return remote(
            source, target, pair_send.at[unit, stream, stage], pair_recv.at[unit, stream, stage],
            {"rep": partners[side]},
        )

    def fs_copy(unit, stream, step):
        p, _, _, slots, _ = views(unit)
        a, b = mine(stream)
        peer = fs_peers[step]
        source = p.at[stream, a, b] if unit == 0 else p.at[stream, a, b, peer]
        return remote(
            source, slots.at[stream, step],
            fs_send.at[unit, stream, step], fs_recv.at[unit, stream, step], {"fs": peer},
        )

    def product(unit):
        if unit == 0:
            @pl.loop(0, blocks)
            def _(block):
                columns = pl.ds(pl.multiple_of(block * width, width), width)
                term = token_dot(conv_out[:, columns], gate_cot[:, columns])
                gate_part[:, :, :, block] = term.reshape(2, 2, 2, gate_rows, width)
        else:
            k = unit - 1
            column, half = k // halves, k % halves
            @pl.loop(0, fs_size)
            def _(owner):
                start = pl.multiple_of(owner * fs_rows + half * half_rows, half_rows)
                term = token_dot(
                    normed[:, pl.ds(start, half_rows)], rec_cot[:, column * width : (column + 1) * width]
                )
                part[k, :, :, :, owner] = term.reshape(2, 2, 2, quarter, width)

    def start_pair(unit, stage):
        for stream in range(2):
            pair_copy(unit, stream, stage).start()

    def add_first(unit):
        p, one, _, _, _ = views(unit)
        for stream in range(2):
            pair_copy(unit, stream, 0).wait_recv()
            a, b = mine(stream)
            @pl.loop(0, p.shape[3])
            def _(i):
                for other in range(2):
                    p[stream, a, other, i] += one[stream, other, i]
            pair_copy(unit, stream, 1).start()

    def add_second(unit):
        p, _, two, _, _ = views(unit)
        for stream in range(2):
            pair_copy(unit, stream, 1).wait_recv()
            a, b = mine(stream)
            @pl.loop(0, p.shape[3])
            def _(i):
                p[stream, a, b, i] += two[stream, i]
            for step in range(fs_size - 1):
                fs_copy(unit, stream, step).start()

    def add_along(unit):
        p, _, _, slots, g = views(unit)
        for stream in range(2):
            a, b = mine(stream)
            for step in range(fs_size - 1):
                fs_copy(unit, stream, step).wait_recv()
            total = p[stream, a, b] if unit == 0 else p[stream, a, b, fs]
            for step in range(fs_size - 1):
                total = total + slots[stream, step]
            g[stream, a, b] = total
            pair_copy(unit, stream, 2).start()

    def forward(unit):
        for stream in range(2):
            pair_copy(unit, stream, 2).wait_recv()
            pair_copy(unit, stream, 3).start()

    def finish(unit):
        for stream in range(2):
            pair_copy(unit, stream, 3).wait_recv()
        if unit == 0:
            @pl.loop(0, blocks)
            def _(block):
                gradient = gate_grad[:, :, :, block].reshape(8 * gate_rows, width)
                right_done = split_dot(gradient, gate_right[block])
                pre = split_dot_left(gate_left[block], right_done)
                gate_pre[block] = pre
                moment = BETA * gate_moment[block] + pre
                sums[2] += folded_squares(gradient) * (1.0 / fs_size)
                sums[3] += folded_squares(moment)
        else:
            k = unit - 1
            column, half = k // halves, k % halves
            columns = slice(column * width, (column + 1) * width)
            rows = slice(half * half_rows, (half + 1) * half_rows)
            gradient = grad[k].reshape(half_rows, width)
            pre = split_dot(gradient, rec_right[columns, :])
            rec_pre[rows, columns] = pre
            moment = BETA * rec_moment[rows, columns] + pre
            sums[0] += folded_squares(gradient)
            sums[1] += folded_squares(moment)

    product(0)
    pl.semaphore_wait(barrier, len(peers))
    stages = (None, add_first, add_second, add_along, forward, finish)
    for tick in range(unit_count + 5):
        if tick < unit_count:
            if tick > 0:
                product(tick)
            start_pair(tick, 0)
        for lag in range(1, 6):
            if 0 <= tick - lag < unit_count:
                stages[lag](tick - lag)

    def exchange(slots, axis, axis_peers, base):
        copies = [
            remote(sums, slots.at[i], sum_send.at[base + i], sum_recv.at[base + i], {axis: peer})
            for i, peer in enumerate(axis_peers)
        ]
        for copy in copies:
            copy.start()
        for copy in copies:
            copy.wait()
        total = sums[...]
        for i in range(len(copies)):
            total = total + slots[i]
        return total

    sums[...] = exchange(sums_fs, "fs", fs_peers, 0)
    total = exchange(sums_tp, "tp", tp_peers, fs_size - 1)
    squares = [jnp.sum(total[i], keepdims=True) for i in range(4)]
    rec_scale = jnp.sqrt(squares[0]) / jnp.sqrt(squares[1] + EPSILON)
    gate_scale = jnp.sqrt(squares[2]) / jnp.sqrt(squares[3] + EPSILON)
    scales[0] = jnp.broadcast_to(rec_scale, (8, LANES))
    scales[1] = jnp.broadcast_to(gate_scale, (8, LANES))

    for unit in range(unit_count):
        for stream in range(2):
            for stage in range(4):
                pair_copy(unit, stream, stage).wait_send()
            for step in range(fs_size - 1):
                fs_copy(unit, stream, step).wait_send()


def shards(fs_size, rep_size, tp_size, normed, rec_cot, conv_out, gate_cot, rec_weight, rec_moment,
           rec_right, gate_weight, gate_moment, gate_left, gate_right):
    assert rep_size == 4
    f32 = jnp.float32
    fs_rows, columns = rec_weight.shape
    width = rec_right.shape[1]
    blocks = gate_weight.shape[0]
    halves = 2 if fs_rows % 256 == 0 else 1
    chunks = columns // width * halves
    quarter = fs_rows // (8 * halves)
    gate_rows = gate_right.shape[1] // 8
    units = chunks + 1
    others = fs_size - 1
    vmem = pl.BlockSpec(memory_space=pltpu.VMEM)
    rec_pre, gate_pre, scales = pl.pallas_call(
        functools.partial(kernel, fs_size, tp_size, halves),
        out_shape=(
            jax.ShapeDtypeStruct(rec_weight.shape, f32),
            jax.ShapeDtypeStruct(gate_weight.shape, f32),
            jax.ShapeDtypeStruct((2, 8, LANES), f32),
        ),
        in_specs=[vmem] * 9,
        out_specs=(vmem,) * 3,
        scratch_shapes=[
            pltpu.VMEM((chunks, 2, 2, 2, fs_size, quarter, width), f32),
            pltpu.VMEM((chunks, 2, 2, fs_size, quarter, width), f32),
            pltpu.VMEM((chunks, 2, fs_size, quarter, width), f32),
            pltpu.VMEM((chunks, 2, others, quarter, width), f32),
            pltpu.VMEM((chunks, 2, 2, 2, quarter, width), f32),
            pltpu.VMEM((2, 2, 2, blocks, gate_rows, width), f32),
            pltpu.VMEM((2, 2, blocks, gate_rows, width), f32),
            pltpu.VMEM((2, blocks, gate_rows, width), f32),
            pltpu.VMEM((2, others, blocks, gate_rows, width), f32),
            pltpu.VMEM((2, 2, 2, blocks, gate_rows, width), f32),
            pltpu.VMEM((4, 8, LANES), f32),
            pltpu.VMEM((others, 4, 8, LANES), f32),
            pltpu.VMEM((tp_size - 1, 4, 8, LANES), f32),
            pltpu.SemaphoreType.DMA((units, 2, 4)),
            pltpu.SemaphoreType.DMA((units, 2, 4)),
            pltpu.SemaphoreType.DMA((units, 2, others)),
            pltpu.SemaphoreType.DMA((units, 2, others)),
            pltpu.SemaphoreType.DMA((others + tp_size - 1,)),
            pltpu.SemaphoreType.DMA((others + tp_size - 1,)),
        ],
        compiler_params=pltpu.CompilerParams(
            collective_id=0, has_side_effects=True, vmem_limit_bytes=60 * 1024 * 1024
        ),
    )(normed, rec_cot, conv_out, gate_cot, rec_moment, rec_right, gate_moment, gate_left, gate_right)

    def update(weight, moment, pre, scale):
        moment_new = BETA * moment + pre
        taken = LEARN_RATE * scale * moment_new
        new = weight - taken
        return new, moment_new, taken, new.astype(jnp.bfloat16)

    return update(rec_weight, rec_moment, rec_pre, scales[0, 0, 0]) + update(
        gate_weight, gate_moment, gate_pre, scales[1, 0, 0]
    )


def solution(mesh):
    in_specs = (
        P(("fs", "rep"), None),
        P(("fs", "rep"), "tp"),
        P(("fs", "rep"), "tp"),
        P(("fs", "rep"), "tp"),
        P("fs", "tp"),
        P("fs", "tp"),
        P("tp", None),
        P("tp", "fs", None),
        P("tp", "fs", None),
        P("tp", "fs", None),
        P("tp", None, None),
    )
    out_specs = (P("fs", "tp"),) * 4 + (P("tp", "fs", None),) * 4
    body = functools.partial(shards, mesh.shape["fs"], mesh.shape["rep"], mesh.shape["tp"])
    return jax.shard_map(body, mesh=mesh, in_specs=in_specs, out_specs=out_specs, check_vma=False)
```

```python
import functools

import jax
import jax.numpy as jnp
from jax import lax
from jax.experimental import pallas as pl
from jax.experimental.pallas import tpu as pltpu
from jax.sharding import PartitionSpec as P

BETA = 0.9
LEARN_RATE = 0.02
EPSILON = 1e-06
MESH = pl.DeviceIdType.MESH
LANES = 128


def split_dot(value, factor):
    high = value.astype(jnp.bfloat16)
    low = (value - high.astype(jnp.float32)).astype(jnp.bfloat16)
    return jnp.dot(high, factor, preferred_element_type=jnp.float32) + jnp.dot(
        low, factor, preferred_element_type=jnp.float32
    )


def split_dot_left(factor, value):
    high = value.astype(jnp.bfloat16)
    low = (value - high.astype(jnp.float32)).astype(jnp.bfloat16)
    return jnp.dot(factor, high, preferred_element_type=jnp.float32) + jnp.dot(
        factor, low, preferred_element_type=jnp.float32
    )


def token_dot(left, right):
    return lax.dot_general(left, right, (((0,), (0,)), ((), ())), preferred_element_type=jnp.float32)


def folded_squares(value):
    squares = value * value
    rows, width = squares.shape
    total = jnp.sum(squares.reshape(rows // 8, 8, width), axis=0)
    result = total[:, :LANES]
    for start in range(LANES, width, LANES):
        result = result + total[:, start : start + LANES]
    return result


def kernel(
    fs_size, tp_size, halves,
    normed, rec_cot, conv_out, gate_cot, rec_moment, rec_right, gate_moment, gate_left, gate_right,
    rec_pre, gate_pre, scales,
    part, first, second, along, grad,
    gate_part, gate_first, gate_second, gate_along, gate_grad,
    sums, sums_fs, sums_tp,
    pair_send, pair_recv, fs_send, fs_recv, sum_send, sum_recv,
):
    fs, rep, tp = lax.axis_index("fs"), lax.axis_index("rep"), lax.axis_index("tp")
    bits = (lax.rem(rep, 2), rep // 2)
    partners = (rep + 1 - 2 * bits[0], rep + 2 - 4 * bits[1])
    fs_peers = [lax.rem(fs + step, fs_size) for step in range(1, fs_size)]
    tp_peers = [lax.rem(tp + step, tp_size) for step in range(1, tp_size)]

    barrier = pltpu.get_barrier_semaphore()
    peers = [{"rep": p} for p in partners] + [{"fs": p} for p in fs_peers] + [{"tp": p} for p in tp_peers]
    for peer in peers:
        pl.semaphore_signal(barrier, inc=1, device_id=peer, device_id_type=MESH)

    chunks = part.shape[0]
    width = part.shape[-1]
    quarter = part.shape[-2]
    half_rows = 8 * quarter
    fs_rows = halves * half_rows
    blocks = gate_part.shape[3]
    gate_rows = gate_part.shape[4]
    unit_count = chunks + 1
    sums[...] = jnp.zeros_like(sums)

    def remote(source, target, send, recv, peer):
        return pltpu.make_async_remote_copy(
            src_ref=source, dst_ref=target, send_sem=send, recv_sem=recv,
            device_id=peer, device_id_type=MESH,
        )

    def views(unit):
        if unit == 0:
            return gate_part, gate_first, gate_second, gate_along, gate_grad
        k = unit - 1
        return part.at[k], first.at[k], second.at[k], along.at[k], grad.at[k]

    def mine(stream):
        return bits[stream], bits[1 - stream]

    def pair_copy(unit, stream, stage):
        p, one, two, _, g = views(unit)
        a, b = mine(stream)
        side = stream if stage in (0, 3) else 1 - stream
        if stage == 0:
            source, target = p.at[stream, 1 - a], one.at[stream]
        elif stage == 1:
            source, target = p.at[stream, a, 1 - b], two.at[stream]
        elif stage == 2:
            source = target = g.at[stream, a, b]
        else:
            source = target = g.at[stream, a]
        return remote(
            source, target, pair_send.at[unit, stream, stage], pair_recv.at[unit, stream, stage],
            {"rep": partners[side]},
        )

    def fs_copy(unit, stream, step):
        p, _, _, slots, _ = views(unit)
        a, b = mine(stream)
        peer = fs_peers[step]
        source = p.at[stream, a, b] if unit == 0 else p.at[stream, a, b, peer]
        return remote(
            source, slots.at[stream, step],
            fs_send.at[unit, stream, step], fs_recv.at[unit, stream, step], {"fs": peer},
        )

    def product(unit):
        if unit == 0:
            @pl.loop(0, blocks)
            def _(block):
                columns = pl.ds(pl.multiple_of(block * width, width), width)
                term = token_dot(conv_out[:, columns], gate_cot[:, columns])
                gate_part[:, :, :, block] = term.reshape(2, 2, 2, gate_rows, width)
        else:
            k = unit - 1
            column, half = k // halves, k % halves
            @pl.loop(0, fs_size)
            def _(owner):
                start = pl.multiple_of(owner * fs_rows + half * half_rows, half_rows)
                term = token_dot(
                    normed[:, pl.ds(start, half_rows)], rec_cot[:, column * width : (column + 1) * width]
                )
                part[k, :, :, :, owner] = term.reshape(2, 2, 2, quarter, width)

    def start_pair(unit, stage):
        for stream in range(2):
            pair_copy(unit, stream, stage).start()

    def add_first(unit):
        p, one, _, _, _ = views(unit)
        for stream in range(2):
            pair_copy(unit, stream, 0).wait_recv()
            a, b = mine(stream)
            @pl.loop(0, p.shape[3])
            def _(i):
                for other in range(2):
                    p[stream, a, other, i] += one[stream, other, i]
            pair_copy(unit, stream, 1).start()

    def add_second(unit):
        p, _, two, _, _ = views(unit)
        for stream in range(2):
            pair_copy(unit, stream, 1).wait_recv()
            a, b = mine(stream)
            @pl.loop(0, p.shape[3])
            def _(i):
                p[stream, a, b, i] += two[stream, i]
            for step in range(fs_size - 1):
                fs_copy(unit, stream, step).start()

    def add_along(unit):
        p, _, _, slots, g = views(unit)
        for stream in range(2):
            a, b = mine(stream)
            for step in range(fs_size - 1):
                fs_copy(unit, stream, step).wait_recv()
            total = p[stream, a, b] if unit == 0 else p[stream, a, b, fs]
            for step in range(fs_size - 1):
                total = total + slots[stream, step]
            g[stream, a, b] = total
            pair_copy(unit, stream, 2).start()

    def forward(unit):
        for stream in range(2):
            pair_copy(unit, stream, 2).wait_recv()
            pair_copy(unit, stream, 3).start()

    def finish(unit):
        for stream in range(2):
            pair_copy(unit, stream, 3).wait_recv()
        if unit == 0:
            @pl.loop(0, blocks)
            def _(block):
                gradient = gate_grad[:, :, :, block].reshape(8 * gate_rows, width)
                right_done = split_dot(gradient, gate_right[block])
                pre = split_dot_left(gate_left[block], right_done)
                gate_pre[block] = pre
                moment = BETA * gate_moment[block] + pre
                sums[2] += folded_squares(gradient) * (1.0 / fs_size)
                sums[3] += folded_squares(moment)
        else:
            k = unit - 1
            column, half = k // halves, k % halves
            columns = slice(column * width, (column + 1) * width)
            rows = slice(half * half_rows, (half + 1) * half_rows)
            gradient = grad[k].reshape(half_rows, width)
            pre = split_dot(gradient, rec_right[columns, :])
            rec_pre[rows, columns] = pre
            moment = BETA * rec_moment[rows, columns] + pre
            sums[0] += folded_squares(gradient)
            sums[1] += folded_squares(moment)

    product(0)
    pl.semaphore_wait(barrier, len(peers))
    stages = (None, add_first, add_second, add_along, forward, finish)
    for tick in range(unit_count + 6):
        if tick < unit_count:
            if tick > 0:
                product(tick)
            start_pair(tick, 0)
        for lag in range(1, 6):
            if 0 <= tick - lag - 1 < unit_count:
                stages[lag](tick - lag - 1)

    def exchange(slots, axis, axis_peers, base):
        copies = [
            remote(sums, slots.at[i], sum_send.at[base + i], sum_recv.at[base + i], {axis: peer})
            for i, peer in enumerate(axis_peers)
        ]
        for copy in copies:
            copy.start()
        for copy in copies:
            copy.wait()
        total = sums[...]
        for i in range(len(copies)):
            total = total + slots[i]
        return total

    sums[...] = exchange(sums_fs, "fs", fs_peers, 0)
    total = exchange(sums_tp, "tp", tp_peers, fs_size - 1)
    squares = [jnp.sum(total[i], keepdims=True) for i in range(4)]
    rec_scale = jnp.sqrt(squares[0]) / jnp.sqrt(squares[1] + EPSILON)
    gate_scale = jnp.sqrt(squares[2]) / jnp.sqrt(squares[3] + EPSILON)
    scales[0] = jnp.broadcast_to(rec_scale, (8, LANES))
    scales[1] = jnp.broadcast_to(gate_scale, (8, LANES))

    for unit in range(unit_count):
        for stream in range(2):
            for stage in range(4):
                pair_copy(unit, stream, stage).wait_send()
            for step in range(fs_size - 1):
                fs_copy(unit, stream, step).wait_send()


def shards(fs_size, rep_size, tp_size, normed, rec_cot, conv_out, gate_cot, rec_weight, rec_moment,
           rec_right, gate_weight, gate_moment, gate_left, gate_right):
    assert rep_size == 4
    f32 = jnp.float32
    fs_rows, columns = rec_weight.shape
    width = rec_right.shape[1]
    blocks = gate_weight.shape[0]
    halves = 2 if fs_rows % 256 == 0 else 1
    chunks = columns // width * halves
    quarter = fs_rows // (8 * halves)
    gate_rows = gate_right.shape[1] // 8
    units = chunks + 1
    others = fs_size - 1
    vmem = pl.BlockSpec(memory_space=pltpu.VMEM)
    rec_pre, gate_pre, scales = pl.pallas_call(
        functools.partial(kernel, fs_size, tp_size, halves),
        out_shape=(
            jax.ShapeDtypeStruct(rec_weight.shape, f32),
            jax.ShapeDtypeStruct(gate_weight.shape, f32),
            jax.ShapeDtypeStruct((2, 8, LANES), f32),
        ),
        in_specs=[vmem] * 9,
        out_specs=(vmem,) * 3,
        scratch_shapes=[
            pltpu.VMEM((chunks, 2, 2, 2, fs_size, quarter, width), f32),
            pltpu.VMEM((chunks, 2, 2, fs_size, quarter, width), f32),
            pltpu.VMEM((chunks, 2, fs_size, quarter, width), f32),
            pltpu.VMEM((chunks, 2, others, quarter, width), f32),
            pltpu.VMEM((chunks, 2, 2, 2, quarter, width), f32),
            pltpu.VMEM((2, 2, 2, blocks, gate_rows, width), f32),
            pltpu.VMEM((2, 2, blocks, gate_rows, width), f32),
            pltpu.VMEM((2, blocks, gate_rows, width), f32),
            pltpu.VMEM((2, others, blocks, gate_rows, width), f32),
            pltpu.VMEM((2, 2, 2, blocks, gate_rows, width), f32),
            pltpu.VMEM((4, 8, LANES), f32),
            pltpu.VMEM((others, 4, 8, LANES), f32),
            pltpu.VMEM((tp_size - 1, 4, 8, LANES), f32),
            pltpu.SemaphoreType.DMA((units, 2, 4)),
            pltpu.SemaphoreType.DMA((units, 2, 4)),
            pltpu.SemaphoreType.DMA((units, 2, others)),
            pltpu.SemaphoreType.DMA((units, 2, others)),
            pltpu.SemaphoreType.DMA((others + tp_size - 1,)),
            pltpu.SemaphoreType.DMA((others + tp_size - 1,)),
        ],
        compiler_params=pltpu.CompilerParams(
            collective_id=0, has_side_effects=True, vmem_limit_bytes=60 * 1024 * 1024
        ),
    )(normed, rec_cot, conv_out, gate_cot, rec_moment, rec_right, gate_moment, gate_left, gate_right)

    def update(weight, moment, pre, scale):
        moment_new = BETA * moment + pre
        taken = LEARN_RATE * scale * moment_new
        new = weight - taken
        return new, moment_new, taken, new.astype(jnp.bfloat16)

    return update(rec_weight, rec_moment, rec_pre, scales[0, 0, 0]) + update(
        gate_weight, gate_moment, gate_pre, scales[1, 0, 0]
    )


def solution(mesh):
    in_specs = (
        P(("fs", "rep"), None),
        P(("fs", "rep"), "tp"),
        P(("fs", "rep"), "tp"),
        P(("fs", "rep"), "tp"),
        P("fs", "tp"),
        P("fs", "tp"),
        P("tp", None),
        P("tp", "fs", None),
        P("tp", "fs", None),
        P("tp", "fs", None),
        P("tp", None, None),
    )
    out_specs = (P("fs", "tp"),) * 4 + (P("tp", "fs", None),) * 4
    body = functools.partial(shards, mesh.shape["fs"], mesh.shape["rep"], mesh.shape["tp"])
    return jax.shard_map(body, mesh=mesh, in_specs=in_specs, out_specs=out_specs, check_vma=False)
```
